32 devices in a mesh: fs: 8 (over z, y), tp: 4 (over x, core).
Axes of the slice: x: 2, y: 2, z: 4, core: 2. Of those that a mesh axis runs over, the one named last changes fastest.
Arguments:
- first_map: bfloat16 [6144, 2048], P('fs', 'tp'), may hold values from -6 to 6
- second_map: bfloat16 [6144, 2048], P('fs', 'tp'), may hold values from -6 to 6
- lambda_head: float32 [16], P('tp'), may hold values from 0.3 to 0.8
- head_gain: float32 [2048], P('tp'), may hold values from 0.1 to 1.9
- cot_output: bfloat16 [6144, 4096], P('fs'), may hold values from -6 to 6
- layer_input: bfloat16 [6144, 4096], P('fs'), may hold values from -6 to 6
- cot_values: bfloat16 [6144, 2048], P('fs', 'tp'), may hold values from -16 to 16
- factor_value: bfloat16 [4096, 256], P('fs'), may hold values from -1 to 1
- factor_output: bfloat16 [4096, 256], P('fs'), may hold values from -1 to 1
- weight_value: float32 [4096, 2048], P('fs', 'tp'), may hold values from -6 to 6
- weight_output: float32 [2048, 4096], P('tp', 'fs'), may hold values from -6 to 6
- first_value: float32 [256, 2048], P('fs', 'tp'), may hold values from -6 to 6
- second_value: float32 [256, 2048], P('fs', 'tp'), may hold values from 0.05 to 1
- first_output: float32 [256, 2048], P('fs', 'tp'), may hold values from -6 to 6
- second_output: float32 [256, 2048], P('fs', 'tp'), may hold values from 0.05 to 1
Outputs:
- new_weight_value: float32 [4096, 2048], P('fs', 'tp')
- new_first_value: float32 [256, 2048], P('fs', 'tp')
- new_second_value: float32 [256, 2048], P('fs', 'tp')
- copy_value: bfloat16 [4096, 2048], P(None, 'tp')
- new_weight_output: float32 [2048, 4096], P('tp', 'fs')
- new_first_output: float32 [256, 2048], P('fs', 'tp')
- new_second_output: float32 [256, 2048], P('fs', 'tp')
- copy_output: bfloat16 [2048, 4096], P('tp')
The draws below stay inside these ranges and needn't reach their ends.
All inputs are finite; a program needn't handle non-finite values.
Results may differ from the reference program's by a relative error of at most 0.002.
Values may be sent and summed in bfloat16 or wider, within the bound.
No kernel may reach another device: no remote copies, remote signals or barrier semaphores. Data moves between devices by JAX's collectives and lax.ppermute only.
A program may use at most 128 MiB of HBM per device.

```python
import math
import jax
import jax.numpy as jnp
from jax import lax

D = 4096
HEADS = 16
RANK = 256
HV = 2048
TOKENS = 6144


def rising_draw(key, count_rows, count_cols, top_scale):
    base = jnp.clip(jax.random.normal(key, (count_rows, count_cols), jnp.float32), -4.0, 4.0)
    column = jnp.arange(count_cols, dtype=jnp.float32) / max(count_cols - 1, 1)
    return base * (top_scale ** column)[None, :]


def draw_cot_values(key, part):
    return rising_draw(jax.random.fold_in(key, 11), TOKENS, HV, 4.0).astype(jnp.bfloat16)


def draw_factor_value(key, part):
    return (rising_draw(jax.random.fold_in(key, 12), D, RANK, 4.0) * RANK ** (-0.5)).astype(jnp.bfloat16)


def draw_factor_output(key, part):
    return (rising_draw(jax.random.fold_in(key, 13), D, RANK, 4.0) * RANK ** (-0.5)).astype(jnp.bfloat16)


def levels(rng, dims, cuts, smallest, high):
    loudness = 1.0
    for dim, parts in cuts:
        heights = jax.random.uniform(jax.random.fold_in(jax.random.fold_in(rng, 6), dim), (parts,), jnp.float32, smallest / len(cuts), high / len(cuts))
        loudness = loudness * jnp.repeat(jnp.exp(heights), dims[dim] // parts).reshape((-1,) + (1,) * (len(dims) - 1 - dim))
    return loudness


def normal_values(stream_key, dims, scale, reach, split=(), kind=jnp.bfloat16):
    result = scale * jax.random.normal(stream_key, dims, jnp.float32)
    if split:
        result = result * levels(stream_key, dims, split, -0.22, 0.18)
    return jnp.clip(result, -reach, reach).astype(kind)


def setup_inputs(seed: int = 0) -> dict:
    keys = jax.random.split(jax.random.key(seed), 16)
    first_map = normal_values(keys[0], (TOKENS, HV), 1.0, 6.0, ((0, 8), (1, 4)))
    second_map = normal_values(keys[1], (TOKENS, HV), 1.0, 6.0, ((0, 8), (1, 4)))
    lambda_head = jnp.clip(0.3 + 0.5 * jax.random.uniform(keys[2], (HEADS,), jnp.float32) ** levels(keys[2], (HEADS,), ((0, 4),), -0.2, 0.2), 0.3, 0.8)
    head_gain = jnp.clip(1.0 + 0.18 * jax.random.normal(keys[3], (HV,), jnp.float32), 0.1, 1.9)
    cot_output = normal_values(keys[4], (TOKENS, D), 1.0, 6.0, ((0, 8),))
    layer_input = normal_values(keys[5], (TOKENS, D), 1.0, 6.0, ((0, 8),))
    cot_values = draw_cot_values(jax.random.fold_in(keys[15], 71), 0)
    factor_value = draw_factor_value(jax.random.fold_in(keys[15], 71), 0)
    factor_output = draw_factor_output(jax.random.fold_in(keys[15], 71), 0)
    weight_value = normal_values(keys[9], (D, HV), 1.0, 6.0, ((0, 8), (1, 4)), jnp.float32)
    weight_output = normal_values(keys[10], (HV, D), 1.0, 6.0, ((0, 4), (1, 8)), jnp.float32)
    first_value = normal_values(keys[11], (RANK, HV), 1.0, 6.0, ((0, 8), (1, 4)), jnp.float32)
    second_value = jnp.clip(jnp.exp(math.log(1.0) - 2.9957323 * jax.random.uniform(keys[12], (RANK, HV), jnp.float32) ** levels(keys[12], (RANK, HV), ((0, 8), (1, 4)), -0.2, 0.2)), 0.05, 1.0)
    first_output = normal_values(keys[13], (RANK, HV), 1.0, 6.0, ((0, 8), (1, 4)), jnp.float32)
    second_output = jnp.clip(jnp.exp(math.log(1.0) - 2.9957323 * jax.random.uniform(keys[14], (RANK, HV), jnp.float32) ** levels(keys[14], (RANK, HV), ((0, 8), (1, 4)), -0.2, 0.2)), 0.05, 1.0)
    return dict(first_map=first_map, second_map=second_map, lambda_head=lambda_head, head_gain=head_gain, cot_output=cot_output, layer_input=layer_input, cot_values=cot_values, factor_value=factor_value, factor_output=factor_output, weight_value=weight_value, weight_output=weight_output, first_value=first_value, second_value=second_value, first_output=first_output, second_output=second_output)


norm_epsilon = 1e-06
first_decay = 0.9
second_decay = 0.95
learn_rate = 0.1

def head_output(first_map, second_map, lambda_head, head_gain):
    heads_here = lambda_head.shape[0]
    head_width = first_map.shape[1] // heads_here
    count_rows = first_map.shape[0]
    spread = jnp.repeat(lambda_head, head_width)
    differ = first_map.astype(jnp.float32) - spread[None, :] * second_map.astype(jnp.float32)
    grouped = differ.reshape(count_rows, heads_here, head_width)
    scaled = grouped * lax.rsqrt(lax.optimization_barrier(jnp.mean(grouped * grouped, -1, keepdims=True)) + norm_epsilon)
    return (scaled.reshape(count_rows, heads_here * head_width) * head_gain[None, :]).astype(jnp.bfloat16)

def moments(projected, clip_factor, first_old, second_old):
    scaled = clip_factor * projected
    first_new = first_decay * first_old + (1.0 - first_decay) * scaled
    second_new = second_decay * second_old + (1.0 - second_decay) * scaled * scaled
    return (first_new, second_new, first_new * lax.rsqrt(second_new))

def reference(first_map, second_map, lambda_head, head_gain, cot_output, layer_input, cot_values, factor_value, factor_output, weight_value, weight_output, first_value, second_value, first_output, second_output):
    heads_out = head_output(first_map, second_map, lambda_head, head_gain)
    mapped_value = jnp.dot(layer_input.astype(jnp.float32), factor_value.astype(jnp.float32), precision=lax.Precision.HIGHEST)
    mapped_output = jnp.dot(cot_output.astype(jnp.float32), factor_output.astype(jnp.float32), precision=lax.Precision.HIGHEST)
    low_value = jnp.dot(mapped_value.T, cot_values.astype(jnp.float32), precision=lax.Precision.HIGHEST)
    low_output = jnp.dot(mapped_output.T, heads_out.astype(jnp.float32), precision=lax.Precision.HIGHEST)
    total = jnp.sum(low_value * low_value) + jnp.sum(low_output * low_output)
    clip_factor = jnp.minimum(1.0, math.sqrt(RANK * HV) * lax.rsqrt(total + norm_epsilon))
    first_v, second_v, ratio_value = moments(low_value, clip_factor, first_value, second_value)
    first_o, second_o, ratio_output = moments(low_output, clip_factor, first_output, second_output)
    update_value = jnp.dot(factor_value.astype(jnp.float32), ratio_value, precision=lax.Precision.HIGHEST)
    update_output = lax.dot_general(ratio_output, factor_output.astype(jnp.float32), (((0,), (1,)), ((), ())), precision=lax.Precision.HIGHEST)
    new_value = weight_value - learn_rate * update_value
    new_output = weight_output - learn_rate * update_output
    return (new_value, first_v, second_v, new_value.astype(jnp.bfloat16), new_output, first_o, second_o, new_output.astype(jnp.bfloat16))
```

```python
import math

import jax
import jax.numpy as jnp
from jax import lax
from jax.sharding import PartitionSpec as P

norm_epsilon = 1e-06
first_decay = 0.9
second_decay = 0.95
learn_rate = 0.1
weight_scale = 2.0**13
ratio_scale = 2.0**10


f32, bf16, f16 = jnp.float32, jnp.bfloat16, jnp.float16


def head_output(first_map, second_map, lambda_head, head_gain):
    heads_here = lambda_head.shape[0]
    head_width = first_map.shape[1] // heads_here
    parts = []
    for h in range(heads_here):
        cols = slice(h * head_width, (h + 1) * head_width)
        differ = first_map[:, cols].astype(f32) - lambda_head[h] * second_map[:, cols].astype(f32)
        scale = lax.rsqrt(jnp.mean(differ * differ, -1, keepdims=True) + norm_epsilon)
        parts.append((differ * scale * head_gain[None, cols]).astype(bf16))
    return jnp.concatenate(parts, axis=1)


def split(x):
    high = lax.reduce_precision(x, 8, 7)
    return high.astype(bf16), (x - high).astype(bf16)


def dot(a, b, dims):
    return lax.dot_general(a, b, (dims, ((), ())), preferred_element_type=f32)


def shift(x, axis, k):
    n = lax.axis_size(axis)
    return lax.ppermute(x, axis, [(i, (i + k) % n) for i in range(n)])


def swap(x, axis, bit):
    n = lax.axis_size(axis)
    return lax.ppermute(x, axis, [(i, i ^ bit) for i in range(n)])


def put(whole, block, index, dim=0):
    return lax.dynamic_update_slice_in_dim(whole, block, index, dim)


def gather_fs(x):
    n = lax.axis_size("fs")
    half = n // 2
    me = lax.axis_index("fs")
    outer, inner = me // 2, me % 2
    mine = jnp.zeros((half,) + x.shape, x.dtype)
    arrived = [shift(x, "fs", 2 * k) for k in range(1, half)]
    mine = put(mine, x[None], outer)
    for k in range(1, half):
        mine = put(mine, arrived[k - 1][None], (outer - k) % half)
    other = swap(mine, "fs", 1)
    lower = jnp.where(inner == 0, mine, other)
    upper = jnp.where(inner == 0, other, mine)
    return jnp.stack([lower, upper], axis=1)


def scatter_fs(x):
    n = lax.axis_size("fs")
    half = n // 2
    me = lax.axis_index("fs")
    outer, inner = me // 2, me % 2
    keep = lax.dynamic_index_in_dim(x, inner, 1, False)
    send = lax.dynamic_index_in_dim(x, 1 - inner, 1, False)
    keep = keep + swap(send, "fs", 1)
    arrived = [
        shift(lax.dynamic_index_in_dim(keep, (outer + k) % half, 0, False), "fs", 2 * k)
        for k in range(1, half)
    ]
    total = lax.dynamic_index_in_dim(keep, outer, 0, False)
    for a in arrived:
        total = total + a
    return total


def gather_tp(x):
    t = lax.axis_size("tp")
    me = lax.axis_index("tp")
    whole = x[None]
    bit = t // 2
    while bit:
        other = swap(whole, "tp", bit)
        low_side = (me // bit) % 2 == 0
        pair = [jnp.where(low_side, whole, other), jnp.where(low_side, other, whole)]
        whole = jnp.stack(pair, axis=1).reshape((-1,) + x.shape)
        bit //= 2
    return whole


def ring_tables():
    n = lax.axis_size("fs")
    order = list(range(0, n, 2)) + list(range(n - 1, 0, -2))
    ahead = [(order[k], order[(k + 1) % n]) for k in range(n)]
    back = [(b, a) for a, b in ahead]
    return ahead, back


def ring_source(steps):
    n = lax.axis_size("fs")
    me = lax.axis_index("fs")
    place = jnp.where(me % 2 == 0, me // 2, n - 1 - me // 2)
    place = (place - steps) % n
    return jnp.where(place < n // 2, 2 * place, 2 * (n - 1 - place) + 1)


def ring_gather(block, dim):
    n = lax.axis_size("fs")
    width = block.shape[dim]
    ahead, back = ring_tables()
    shape = list(block.shape)
    shape[dim] *= n
    whole = jnp.zeros(shape, block.dtype)
    whole = put(whole, block, lax.axis_index("fs") * width, dim)
    down = up = block
    for s in range(1, n // 2):
        down = lax.ppermute(down, "fs", ahead)
        up = lax.ppermute(up, "fs", back)
        whole = put(whole, down, ring_source(s) * width, dim)
        whole = put(whole, up, ring_source(-s) * width, dim)
    rows = block.shape[0] // 2
    far = ring_source(n // 2)
    down = lax.ppermute(down[:rows], "fs", ahead)
    up = lax.ppermute(up[rows:], "fs", back)
    whole = put(whole, jnp.concatenate([down, up], axis=0), far * width, dim)
    return whole


def moments(projected, clip_factor, first_old, second_old):
    scaled = clip_factor * projected
    first_new = first_decay * first_old + (1.0 - first_decay) * scaled
    second_new = second_decay * second_old + (1.0 - second_decay) * scaled * scaled
    return first_new, second_new, first_new * lax.rsqrt(second_new)


def shards(
    first_map,
    second_map,
    lambda_head,
    head_gain,
    cot_output,
    layer_input,
    cot_values,
    factor_value,
    factor_output,
    weight_value,
    weight_output,
    first_value,
    second_value,
    first_output,
    second_output,
):
    n, t = lax.axis_size("fs"), lax.axis_size("tp")
    column = lax.axis_index("tp")
    rank = factor_value.shape[1]
    part = rank // t
    width = factor_value.shape[0] * n

    wide_value = ring_gather((weight_value * weight_scale).astype(f16), 0)
    wide_output = ring_gather((weight_output * weight_scale).astype(f16), 1)

    own = jnp.concatenate(
        [
            lax.dynamic_slice_in_dim(factor_value, column * part, part, 1),
            lax.dynamic_slice_in_dim(factor_output, column * part, part, 1),
        ],
        axis=1,
    )
    piece = gather_fs(own).reshape(width, 2 * part)
    mapped = jnp.where(
        (jnp.arange(2 * part) < part)[None, :],
        dot(layer_input, piece, ((1,), (0,))),
        dot(cot_output, piece, ((1,), (0,))),
    )
    mapped = gather_tp(mapped)
    pieces = gather_tp(piece)
    heads_out = head_output(first_map, second_map, lambda_head, head_gain)

    def low_rank(lanes, right):
        left = jnp.concatenate([mapped[c, :, lanes] for c in range(t)], axis=1)
        high, low = split(left)
        total = dot(high, right, ((0,), (0,))) + dot(low, right, ((0,), (0,)))
        return total.reshape(n // 2, 2, rank // n, right.shape[1])

    value, output = slice(0, part), slice(part, 2 * part)
    partial = jnp.stack([low_rank(value, cot_values), low_rank(output, heads_out)], axis=2)
    low = scatter_fs(partial)
    square = jnp.sum(low * low)
    squares = lax.all_to_all(
        jnp.broadcast_to(square, (n * t, 1, 128)), ("fs", "tp"), 0, 0, tiled=False
    )
    total = jnp.sum(squares[:, 0, 0])
    clip_factor = jnp.minimum(1.0, math.sqrt(rank * cot_values.shape[1] * t) * lax.rsqrt(total + norm_epsilon))
    first_v, second_v, ratio_value = moments(low[0], clip_factor, first_value, second_value)
    first_o, second_o, ratio_output = moments(low[1], clip_factor, first_output, second_output)

    ratio = jnp.stack([ratio_value, ratio_output]) * ratio_scale
    ratios = gather_fs(ratio.astype(f16)).reshape(n, 2, rank // n, -1).astype(f32)
    ratios = ratios * (-learn_rate / ratio_scale)

    def step(which):
        high, low = split(ratios[:, which].reshape(rank, -1))
        return jnp.concatenate([high, low], axis=0)

    step_value, step_output = step(0), step(1)

    def twice(x):
        return jnp.concatenate([x, x], axis=1)

    new_value = weight_value + dot(twice(factor_value), step_value, ((1,), (0,)))
    new_output = weight_output + dot(step_output, twice(factor_output), ((0,), (1,)))
    whole_value = jnp.concatenate([pieces[c, :, value] for c in range(t)], axis=1)
    whole_output = jnp.concatenate([pieces[c, :, output] for c in range(t)], axis=1)
    copy_value = wide_value.astype(f32) * (1.0 / weight_scale) + dot(
        twice(whole_value), step_value, ((1,), (0,))
    )
    copy_output = wide_output.astype(f32) * (1.0 / weight_scale) + dot(
        step_output, twice(whole_output), ((0,), (1,))
    )
    return (
        new_value,
        first_v,
        second_v,
        copy_value.astype(bf16),
        new_output,
        first_o,
        second_o,
        copy_output.astype(bf16),
    )


def solution(mesh):
    placed = (
        P("fs", "tp"),
        P("fs", "tp"),
        P("tp"),
        P("tp"),
        P("fs", None),
        P("fs", None),
        P("fs", "tp"),
        P("fs", None),
        P("fs", None),
        P("fs", "tp"),
        P("tp", "fs"),
        P("fs", "tp"),
        P("fs", "tp"),
        P("fs", "tp"),
        P("fs", "tp"),
    )
    return jax.shard_map(
        shards,
        mesh=mesh,
        in_specs=placed,
        out_specs=(
            P("fs", "tp"),
            P("fs", "tp"),
            P("fs", "tp"),
            P(None, "tp"),
            P("tp", "fs"),
            P("fs", "tp"),
            P("fs", "tp"),
            P("tp", None),
        ),
        check_vma=False,
    )
```

```python
import math

import jax
import jax.numpy as jnp
from jax import lax
from jax.experimental import pallas as pl
from jax.experimental.pallas import tpu as pltpu
from jax.sharding import PartitionSpec as P


norm_epsilon = 1e-06
first_decay = 0.9
second_decay = 0.95
learn_rate = 0.1
weight_scale = 2.0**13
ratio_scale = 2.0**10


f32, bf16, f16 = jnp.float32, jnp.bfloat16, jnp.float16


SMEM = pl.BlockSpec(memory_space=pltpu.SMEM)
VMEM = pl.BlockSpec(memory_space=pltpu.VMEM)


def head_output(first_map, second_map, lambda_head, head_gain):
    heads_here = lambda_head.shape[0]
    count, cols = first_map.shape
    head_width = cols // heads_here
    parts = 8
    rows = count // parts

    def kernel(spread, first, second, gain, out):
        @pl.loop(0, parts)
        def _(p):
            span = pl.ds(pl.multiple_of(p * rows, rows), rows)
            for h in range(heads_here):
                lanes = slice(h * head_width, (h + 1) * head_width)
                differ = first[span, lanes].astype(f32) - spread[h] * second[span, lanes].astype(f32)
                mean = jnp.mean(differ * differ, -1, keepdims=True)
                scaled = differ * lax.rsqrt(mean + norm_epsilon) * gain[:, lanes]
                out[span, lanes] = scaled.astype(bf16)

    return pl.pallas_call(
        kernel,
        out_shape=jax.ShapeDtypeStruct((count, cols), bf16),
        in_specs=[SMEM, VMEM, VMEM, VMEM],
        out_specs=VMEM,
        cost_estimate=pl.CostEstimate(flops=2000 * count * cols, bytes_accessed=6 * count * cols, transcendentals=0),
        compiler_params=pltpu.CompilerParams(vmem_limit_bytes=8 * 2**20),
        name="head_output",
    )(lambda_head, first_map, second_map, head_gain[None])


def split(x):
    high = lax.reduce_precision(x, 8, 7)
    return high.astype(bf16), (x - high).astype(bf16)


def dot(a, b, dims):
    return lax.dot_general(a, b, (dims, ((), ())), preferred_element_type=f32)


def shift(x, axis, k):
    n = lax.axis_size(axis)
    return lax.ppermute(x, axis, [(i, (i + k) % n) for i in range(n)])


def swap(x, axis, bit):
    n = lax.axis_size(axis)
    return lax.ppermute(x, axis, [(i, i ^ bit) for i in range(n)])


def put(whole, block, index, dim=0):
    return lax.dynamic_update_slice_in_dim(whole, block, index, dim)


def blocks_fs(x):
    n = lax.axis_size("fs")
    half = n // 2
    me = lax.axis_index("fs")
    outer, inner = me // 2, me % 2
    line = [x] + [shift(x, "fs", 2 * k) for k in range(1, half)]
    across = [swap(block, "fs", 1) for block in line]
    places = [(outer - k) % half * 2 for k in range(half)]
    return line + across, [p + inner for p in places] + [p + 1 - inner for p in places]


def blocks_tp(x):
    t = lax.axis_size("tp")
    bit = t // 2
    found = {0: x}
    while bit:
        for r in sorted(found):
            found[r | bit] = swap(found[r], "tp", bit)
        bit //= 2
    return [found[r] for r in range(t)]


def gather_fs(x):
    n = lax.axis_size("fs")
    half = n // 2
    me = lax.axis_index("fs")
    outer, inner = me // 2, me % 2
    arrived = [x[None]] + [shift(x, "fs", 2 * k)[None] for k in range(1, half)]
    turned = arrived[:0:-1] + arrived[:1] + arrived[:0:-1]
    mine = lax.dynamic_slice_in_dim(jnp.concatenate(turned, axis=0), half - 1 - outer, half, 0)
    other = swap(mine, "fs", 1)
    lower = jnp.where(inner == 0, mine, other)
    upper = jnp.where(inner == 0, other, mine)
    return jnp.stack([lower, upper], axis=1)


def map_tokens(blocks, places, which, tokens):
    n = len(blocks)
    count, width = tokens[0].shape
    deep, part = blocks[0].shape

    def kernel(at, *refs):
        block_refs, token_refs = refs[:n], refs[n : n + 2]
        product, whole = refs[n + 2 :]
        spans = [pl.ds(pl.multiple_of(at[b] * deep, deep), deep) for b in range(n)]
        for w, held in enumerate(token_refs):

            @pl.when(at[n] == w)
            def _():
                total = jnp.zeros((count, part), f32)
                for b in range(n):
                    total += jnp.dot(held[:, spans[b]], block_refs[b][...], preferred_element_type=f32)
                product[...] = total.T

        for b in range(n):
            whole[spans[b], :] = block_refs[b][...]

    at = jnp.stack([p.astype(jnp.int32) for p in places + [which]])
    return pl.pallas_call(
        kernel,
        out_shape=(
            jax.ShapeDtypeStruct((part, count), f32),
            jax.ShapeDtypeStruct((width, part), bf16),
        ),
        in_specs=[SMEM] + [VMEM] * (n + 2),
        out_specs=(VMEM, VMEM),
        cost_estimate=pl.CostEstimate(flops=2 * count * width * 256, bytes_accessed=2 * count * width, transcendentals=0),
        compiler_params=pltpu.CompilerParams(vmem_limit_bytes=28 * 2**20),
        name="map_tokens",
    )(at, *blocks, *tokens)


def low_rank(mapped, rights):
    t, n = lax.axis_size("tp"), lax.axis_size("fs")
    part, count = mapped[0].shape
    cols = rights[0].shape[1]
    rank = part * t // 2
    rows = rank // n

    def kernel(at, *refs):
        mapped_refs, right_refs = refs[:t], refs[t : t + 2]
        keep, send, peak, both, total = refs[t + 2 :]
        for m in range(2):
            both[m] = right_refs[m][...]
        for r in range(t):
            m, h = at[r] // (t // 2), at[r] % (t // 2)
            x = mapped_refs[r][...]
            high = x.astype(bf16)
            low = (x - high.astype(f32)).astype(bf16)
            right = both[m]
            total[m, pl.ds(pl.multiple_of(h * part, part), part), :] = jnp.dot(
                high, right, preferred_element_type=f32
            ) + jnp.dot(low, right, preferred_element_type=f32)
        top = jnp.zeros((8, cols), f32)
        for m in range(2):
            tall = jnp.abs(total[m])
            top = jnp.maximum(top, jnp.max(tall.reshape(rank // 8, 8, cols), axis=0))
        peak[...] = jnp.max(top, axis=(0, 1), keepdims=True) + jnp.zeros((8, 128), f32)
        for o in range(n // 2):
            for m in range(2):
                first = pl.multiple_of((2 * o + at[t]) * rows, rows)
                keep[o, m] = total[m, pl.ds(first, rows), :]
                other = pl.multiple_of((2 * o + 1 - at[t]) * rows, rows)
                send[o, m] = total[m, pl.ds(other, rows), :]

    me = lax.axis_index("tp")
    at = jnp.stack([me ^ r for r in range(t)] + [lax.axis_index("fs") % 2]).astype(jnp.int32)
    shape = jax.ShapeDtypeStruct((n // 2, 2, rows, cols), f32)
    return pl.pallas_call(
        kernel,
        out_shape=(shape, shape, jax.ShapeDtypeStruct((8, 128), f32)),
        in_specs=[SMEM] + [VMEM] * (t + 2),
        out_specs=(VMEM, VMEM, VMEM),
        scratch_shapes=[pltpu.VMEM((2, count, cols), bf16), pltpu.VMEM((2, rank, cols), f32)],
        cost_estimate=pl.CostEstimate(flops=8 * count * rank * cols, bytes_accessed=4 * rank * cols, transcendentals=0),
        name="low_rank",
    )(at, *mapped, *rights)


def scale_of(peak):
    return jnp.clip(jnp.floor(14.0 - jnp.log2(jnp.maximum(peak, 1e-30))), -100.0, 100.0)


def pack(x, power):
    body = (x * jnp.exp2(power)).astype(f16).reshape(-1, x.shape[-1])
    return jnp.concatenate([body, jnp.full((8, x.shape[-1]), power).astype(f16)], axis=0)


def unpack(packed, shape):
    power = packed[-1, 0].astype(f32)
    return packed[:-8].astype(f32).reshape(shape) * jnp.exp2(-power), power


def add_blocks(keep, came):
    half = keep.shape[0]

    def kernel(at, a, b, *outs):
        for k in range(half):
            o = (at[0] + k) % half
            outs[k][...] = a[o] + b[o]

    at = jnp.stack([lax.axis_index("fs") // 2]).astype(jnp.int32)
    shape = jax.ShapeDtypeStruct(keep.shape[1:], f32)
    return pl.pallas_call(
        kernel,
        out_shape=(shape,) * half,
        in_specs=[SMEM, VMEM, VMEM],
        out_specs=(VMEM,) * half,
        cost_estimate=pl.CostEstimate(flops=keep.size, bytes_accessed=8 * keep.size, transcendentals=0),
        name="add_blocks",
    )(at, keep, came)


def ring_tables():
    n = lax.axis_size("fs")
    order = list(range(0, n, 2)) + list(range(n - 1, 0, -2))
    ahead = [(order[k], order[(k + 1) % n]) for k in range(n)]
    back = [(b, a) for a, b in ahead]
    return ahead, back


def ring_source(steps):
    n = lax.axis_size("fs")
    me = lax.axis_index("fs")
    place = jnp.where(me % 2 == 0, me // 2, n - 1 - me // 2)
    place = (place - steps) % n
    return jnp.where(place < n // 2, 2 * place, 2 * (n - 1 - place) + 1)


class Ring:
    def __init__(self, value, output):
        n = lax.axis_size("fs")
        self.shapes = (value.shape, output.shape)
        self.ahead, self.back = ring_tables()
        self.down = self.up = jnp.stack([value, output.reshape(value.shape)])
        self.steps = n // 2
        self.step = 0
        self.blocks = [(lax.axis_index("fs"), value, output)]

    def start(self):
        self.step += 1
        self.send()
        self.keep()

    def send(self):
        if self.step < self.steps:
            self.down = lax.ppermute(self.down, "fs", self.ahead)
            self.up = lax.ppermute(self.up, "fs", self.back)
        else:
            self.down = lax.ppermute(self.down[0], "fs", self.ahead)
            self.up = lax.ppermute(self.up[1], "fs", self.back)

    def keep(self):
        s = self.step
        if s < self.steps:
            for k, block in ((s, self.down), (-s, self.up)):
                self.blocks.append((ring_source(k), block[0], block[1].reshape(self.shapes[1])))
        else:
            self.blocks.append((ring_source(s), self.down, self.up.reshape(self.shapes[1])))

    def empty(self, after):
        n = lax.axis_size("fs")
        (rows, inner), (outer, cols) = self.shapes
        index, value, output = self.blocks[0]
        value, output, _ = lax.optimization_barrier((value, output, after))
        return (
            put(jnp.zeros((rows * n, inner), f16), value, index * rows, 0),
            put(jnp.zeros((outer, cols * n), f16), output, index * cols, 1),
        )

    def whole(self, value, output):
        rows, cols = self.shapes[0][0], self.shapes[1][1]
        for index, v, o in self.blocks[1:-1]:
            value = put(value, v, index * rows, 0)
            output = put(output, o, index * cols, 1)
        return value, output


def moments(projected, clip_factor, first_old, second_old):
    scaled = clip_factor * projected
    first_new = first_decay * first_old + (1.0 - first_decay) * scaled
    second_new = second_decay * second_old + (1.0 - second_decay) * scaled * scaled
    return first_new, second_new, first_new * lax.rsqrt(second_new)


def update(
    first_map,
    second_map,
    lambda_head,
    head_gain,
    cot_output,
    layer_input,
    cot_values,
    factor_value,
    factor_output,
    weight_value,
    weight_output,
    first_value,
    second_value,
    first_output,
    second_output,
):
    n, t = lax.axis_size("fs"), lax.axis_size("tp")
    column = lax.axis_index("tp")
    rank = factor_value.shape[1]
    part = 2 * rank // t
    half = t // 2

    first = column % half * part
    own = jnp.where(
        column < half,
        lax.dynamic_slice_in_dim(factor_value, first, part, 1),
        lax.dynamic_slice_in_dim(factor_output, first, part, 1),
    )
    blocks, places = blocks_fs(own)
    ring = Ring((weight_value * weight_scale).astype(f16), (weight_output * weight_scale).astype(f16))
    while ring.step < ring.steps:
        ring.start()
    lines, first_map, second_map = lax.optimization_barrier((blocks[: n // 2], first_map, second_map))
    blocks = lines + blocks[n // 2 :]
    heads_out = head_output(first_map, second_map, lambda_head, head_gain)
    mapped, piece = map_tokens(blocks, places, column // half, (layer_input, cot_output))
    wides = ring.empty(mapped)
    mapped = blocks_tp(mapped)
    keep, send, peak = low_rank(mapped, (cot_values, heads_out))
    peak = peak[0, 0]
    packed = pack(send, scale_of(peak))
    packed = swap(packed, "fs", 1)
    came, power = unpack(packed, send.shape)
    power = scale_of(peak + jnp.exp2(15.0 - power))
    pieces = blocks_tp(piece)
    sums = add_blocks(keep, came)
    packed = [pack(sums[k], power) for k in range(1, n // 2)]
    packed = [shift(p, "fs", 2 * (k + 1)) for k, p in enumerate(packed)]
    low = sums[0]
    for p in packed:
        low = low + unpack(p, low.shape)[0]
    square = jnp.sum(low * low)
    squares = lax.all_to_all(
        jnp.broadcast_to(square, (n * t, 1, 128)), ("fs", "tp"), 0, 0, tiled=False
    )
    pieces = jnp.stack(pieces)
    pieces = jnp.stack([pieces[column ^ c] for c in range(t)])
    pieces, squares = lax.optimization_barrier((pieces, squares))
    total = jnp.sum(squares[:, 0, 0])
    clip_factor = jnp.minimum(1.0, math.sqrt(rank * cot_values.shape[1] * t) * lax.rsqrt(total + norm_epsilon))
    first_v, second_v, ratio_value = moments(low[0], clip_factor, first_value, second_value)
    first_o, second_o, ratio_output = moments(low[1], clip_factor, first_output, second_output)

    ratio = jnp.stack([ratio_value, ratio_output]) * ratio_scale
    ratios = gather_fs(ratio.astype(f16)).reshape(n, 2, rank // n, -1).astype(f32)
    ratios = ratios * (-learn_rate / ratio_scale)

    def step(which):
        high, low = split(ratios[:, which].reshape(rank, -1))
        return jnp.concatenate([high, low], axis=0)

    step_value, step_output = step(0), step(1)

    def twice(x):
        return jnp.concatenate([x, x], axis=1)

    wide_value, wide_output = ring.whole(*wides)
    new_value = weight_value + dot(twice(factor_value), step_value, ((1,), (0,)))
    new_output = weight_output + dot(step_output, twice(factor_output), ((0,), (1,)))
    whole_value = jnp.concatenate([pieces[c] for c in range(half)] * 2, axis=1)
    whole_output = jnp.concatenate([pieces[c] for c in range(half, t)] * 2, axis=1)

    def value_rows(held, factor):
        return (held.astype(f32) * (1.0 / weight_scale) + dot(factor, step_value, ((1,), (0,)))).astype(bf16)

    def output_cols(held, factor):
        return (held.astype(f32) * (1.0 / weight_scale) + dot(step_output, factor, ((0,), (1,)))).astype(bf16)

    copy_value = value_rows(wide_value, whole_value)
    copy_output = output_cols(wide_output, whole_output)
    index, far_value, far_output = ring.blocks[-1]
    rows, cols = far_value.shape[0], far_output.shape[1]
    far_value, far_output, copy_value, copy_output = lax.optimization_barrier(
        (far_value, far_output, copy_value, copy_output)
    )

    def rows_of(factor, count):
        return lax.dynamic_slice_in_dim(factor, index * count, count, 0)

    copy_value = put(copy_value, value_rows(far_value, rows_of(whole_value, rows)), index * rows, 0)
    copy_output = put(copy_output, output_cols(far_output, rows_of(whole_output, cols)), index * cols, 1)
    return (
        new_value,
        first_v,
        second_v,
        copy_value,
        new_output,
        first_o,
        second_o,
        copy_output,
    )


def solution(mesh):
    placed = (
        P("fs", "tp"),
        P("fs", "tp"),
        P("tp"),
        P("tp"),
        P("fs", None),
        P("fs", None),
        P("fs", "tp"),
        P("fs", None),
        P("fs", None),
        P("fs", "tp"),
        P("tp", "fs"),
        P("fs", "tp"),
        P("fs", "tp"),
        P("fs", "tp"),
        P("fs", "tp"),
    )
    return jax.shard_map(
        update,
        mesh=mesh,
        in_specs=placed,
        out_specs=(
            P("fs", "tp"),
            P("fs", "tp"),
            P("fs", "tp"),
            P(None, "tp"),
            P("tp", "fs"),
            P("fs", "tp"),
            P("fs", "tp"),
            P("tp", None),
        ),
        check_vma=False,
    )
```

```python
import math

import jax
import jax.numpy as jnp
from jax import lax
from jax.experimental import pallas as pl
from jax.experimental.pallas import tpu as pltpu
from jax.sharding import PartitionSpec as P


norm_epsilon = 1e-06
first_decay = 0.9
second_decay = 0.95
learn_rate = 0.1
weight_scale = 2.0**13
ratio_scale = 2.0**10


f32, bf16, f16 = jnp.float32, jnp.bfloat16, jnp.float16


SMEM = pl.BlockSpec(memory_space=pltpu.SMEM)
VMEM = pl.BlockSpec(memory_space=pltpu.VMEM)
ANY = pl.BlockSpec(memory_space=pl.ANY)


def head_output(first_map, second_map, lambda_head, head_gain):
    heads_here = lambda_head.shape[0]
    count, cols = first_map.shape
    head_width = cols // heads_here
    parts = 8
    rows = count // parts

    def kernel(spread, first, second, gain, out):
        @pl.loop(0, parts)
        def _(p):
            span = pl.ds(pl.multiple_of(p * rows, rows), rows)
            for h in range(heads_here):
                lanes = slice(h * head_width, (h + 1) * head_width)
                differ = first[span, lanes].astype(f32) - spread[h] * second[span, lanes].astype(f32)
                mean = jnp.mean(differ * differ, -1, keepdims=True)
                scaled = differ * lax.rsqrt(mean + norm_epsilon) * gain[:, lanes]
                out[span, lanes] = scaled.astype(bf16)

    return pl.pallas_call(
        kernel,
        out_shape=jax.ShapeDtypeStruct((count, cols), bf16),
        in_specs=[SMEM, VMEM, VMEM, VMEM],
        out_specs=VMEM,
        cost_estimate=pl.CostEstimate(flops=2000 * count * cols, bytes_accessed=6 * count * cols, transcendentals=0),
        compiler_params=pltpu.CompilerParams(vmem_limit_bytes=8 * 2**20),
        name="head_output",
    )(lambda_head, first_map, second_map, head_gain[None])


def split(x):
    high = lax.reduce_precision(x, 8, 7)
    return high.astype(bf16), (x - high).astype(bf16)


def dot(a, b, dims):
    return lax.dot_general(a, b, (dims, ((), ())), preferred_element_type=f32)


def shift(x, axis, k):
    n = lax.axis_size(axis)
    return lax.ppermute(x, axis, [(i, (i + k) % n) for i in range(n)])


def swap(x, axis, bit):
    n = lax.axis_size(axis)
    return lax.ppermute(x, axis, [(i, i ^ bit) for i in range(n)])


def put(whole, block, index, dim=0):
    return lax.dynamic_update_slice_in_dim(whole, block, index, dim)


def blocks_fs(x):
    n = lax.axis_size("fs")
    half = n // 2
    me = lax.axis_index("fs")
    outer, inner = me // 2, me % 2
    line = [x] + [shift(x, "fs", 2 * k) for k in range(1, half)]
    across = [swap(block, "fs", 1) for block in line]
    places = [(outer - k) % half * 2 for k in range(half)]
    return line + across, [p + inner for p in places] + [p + 1 - inner for p in places]


def blocks_tp(x):
    t = lax.axis_size("tp")
    bit = t // 2
    found = {0: x}
    while bit:
        for r in sorted(found):
            found[r | bit] = swap(found[r], "tp", bit)
        bit //= 2
    return [found[r] for r in range(t)]


def gather_fs(x):
    n = lax.axis_size("fs")
    half = n // 2
    me = lax.axis_index("fs")
    outer, inner = me // 2, me % 2
    arrived = [x[None]] + [shift(x, "fs", 2 * k)[None] for k in range(1, half)]
    turned = arrived[:0:-1] + arrived[:1] + arrived[:0:-1]
    mine = lax.dynamic_slice_in_dim(jnp.concatenate(turned, axis=0), half - 1 - outer, half, 0)
    other = swap(mine, "fs", 1)
    lower = jnp.where(inner == 0, mine, other)
    upper = jnp.where(inner == 0, other, mine)
    return jnp.stack([lower, upper], axis=1)


def map_tokens(blocks, places, which, tokens):
    n = len(blocks)
    count, width = tokens[0].shape
    deep, part = blocks[0].shape

    parts = 4
    rows = count // parts

    def kernel(at, *refs):
        block_refs, token_refs = refs[:n], refs[n : n + 2]
        product, whole, held, sems = refs[n + 2 :]
        spans = [pl.ds(pl.multiple_of(at[b] * deep, deep), deep) for b in range(n)]

        def fetch(source, p):
            here = pl.ds(p * rows, rows)
            return pltpu.make_async_copy(source.at[here], held.at[here], sems.at[p])

        for w in range(2):

            @pl.when(at[n] == w)
            def _():
                for p in range(parts):
                    fetch(token_refs[w], p).start()

        for b in range(n):
            whole[spans[b], :] = block_refs[b][...]
        for p in range(parts):
            fetch(token_refs[0], p).wait()
            here = slice(p * rows, (p + 1) * rows)
            total = jnp.dot(held[here], whole[...], preferred_element_type=f32)
            product[here, :] = total

    at = jnp.stack([p.astype(jnp.int32) for p in places + [which]])
    return pl.pallas_call(
        kernel,
        out_shape=(
            jax.ShapeDtypeStruct((count, part), f32),
            jax.ShapeDtypeStruct((width, part), bf16),
        ),
        in_specs=[SMEM] + [VMEM] * n + [ANY] * 2,
        out_specs=(VMEM, VMEM),
        scratch_shapes=[pltpu.VMEM((count, width), bf16), pltpu.SemaphoreType.DMA((parts,))],
        cost_estimate=pl.CostEstimate(flops=2 * count * width * 256, bytes_accessed=2 * count * width, transcendentals=0),
        name="map_tokens",
    )(at, *blocks, *tokens)


def low_rank(mapped, rights):
    t, n = lax.axis_size("tp"), lax.axis_size("fs")
    count, part = mapped[0].shape
    cols = rights[0].shape[1]
    rank = part * t // 2
    rows = rank // n

    def kernel(at, *refs):
        mapped_refs, right_refs = refs[:t], refs[t : t + 2]
        keep, send, peak, both, total = refs[t + 2 :]
        for m in range(2):
            both[m] = right_refs[m][...]
        for r in range(t):
            m, h = at[r] // (t // 2), at[r] % (t // 2)
            x = mapped_refs[r][...].T
            high = x.astype(bf16)
            low = (x - high.astype(f32)).astype(bf16)
            right = both[m]
            total[m, pl.ds(pl.multiple_of(h * part, part), part), :] = jnp.dot(
                high, right, preferred_element_type=f32
            ) + jnp.dot(low, right, preferred_element_type=f32)
        top = jnp.zeros((8, cols), f32)
        for m in range(2):
            tall = jnp.abs(total[m])
            top = jnp.maximum(top, jnp.max(tall.reshape(rank // 8, 8, cols), axis=0))
        peak[...] = jnp.max(top, axis=(0, 1), keepdims=True) + jnp.zeros((8, cols), f32)
        for o in range(n // 2):
            for m in range(2):
                first = pl.multiple_of((2 * o + at[t]) * rows, rows)
                keep[o, m] = total[m, pl.ds(first, rows), :]
                other = pl.multiple_of((2 * o + 1 - at[t]) * rows, rows)
                send[o, m] = total[m, pl.ds(other, rows), :]

    me = lax.axis_index("tp")
    at = jnp.stack([me ^ r for r in range(t)] + [lax.axis_index("fs") % 2]).astype(jnp.int32)
    shape = jax.ShapeDtypeStruct((n // 2, 2, rows, cols), f32)
    return pl.pallas_call(
        kernel,
        out_shape=(shape, shape, jax.ShapeDtypeStruct((8, cols), f32)),
        in_specs=[SMEM] + [VMEM] * (t + 2),
        out_specs=(VMEM, VMEM, VMEM),
        scratch_shapes=[pltpu.VMEM((2, count, cols), bf16), pltpu.VMEM((2, rank, cols), f32)],
        cost_estimate=pl.CostEstimate(flops=8 * count * rank * cols, bytes_accessed=4 * rank * cols, transcendentals=0),
        name="low_rank",
    )(at, *mapped, *rights)


def scale_of(peak):
    return jnp.clip(jnp.floor(14.0 - jnp.log2(jnp.maximum(peak, 1e-30))), -100.0, 100.0)


def pack(x, power):
    body = (x.reshape(-1, x.shape[-1]) * jnp.exp2(power[:1])).astype(f16)
    return jnp.concatenate([body, power.astype(f16)], axis=0)


def unpack(packed, shape):
    power = packed[-8:].astype(f32)
    return (packed[:-8].astype(f32) * jnp.exp2(-power[:1])).reshape(shape), power


def add_blocks(keep, came):
    half = keep.shape[0]

    def kernel(at, a, b, *outs):
        for k in range(half):
            o = (at[0] + k) % half
            outs[k][...] = a[o] + b[o]

    at = jnp.stack([lax.axis_index("fs") // 2]).astype(jnp.int32)
    shape = jax.ShapeDtypeStruct(keep.shape[1:], f32)
    return pl.pallas_call(
        kernel,
        out_shape=(shape,) * half,
        in_specs=[SMEM, VMEM, VMEM],
        out_specs=(VMEM,) * half,
        cost_estimate=pl.CostEstimate(flops=keep.size, bytes_accessed=8 * keep.size, transcendentals=0),
        name="add_blocks",
    )(at, keep, came)


def ring_tables():
    n = lax.axis_size("fs")
    order = list(range(0, n, 2)) + list(range(n - 1, 0, -2))
    ahead = [(order[k], order[(k + 1) % n]) for k in range(n)]
    back = [(b, a) for a, b in ahead]
    return ahead, back


def ring_source(steps):
    n = lax.axis_size("fs")
    me = lax.axis_index("fs")
    place = jnp.where(me % 2 == 0, me // 2, n - 1 - me // 2)
    place = (place - steps) % n
    return jnp.where(place < n // 2, 2 * place, 2 * (n - 1 - place) + 1)


class Ring:
    def __init__(self, value, output):
        n = lax.axis_size("fs")
        self.shapes = (value.shape, output.shape)
        self.ahead, self.back = ring_tables()
        self.down = self.up = jnp.stack([value, output.reshape(value.shape)])
        self.steps = n // 2
        self.step = 0
        self.blocks = [(lax.axis_index("fs"), value, output)]

    def start(self):
        self.step += 1
        self.send()
        self.keep()

    def send(self):
        if self.step < self.steps:
            self.down = lax.ppermute(self.down, "fs", self.ahead)
            self.up = lax.ppermute(self.up, "fs", self.back)
        else:
            self.down = lax.ppermute(self.down[0], "fs", self.ahead)
            self.up = lax.ppermute(self.up[1], "fs", self.back)

    def keep(self):
        s = self.step
        if s < self.steps:
            for k, block in ((s, self.down), (-s, self.up)):
                self.blocks.append((ring_source(k), block[0], block[1].reshape(self.shapes[1])))
        else:
            self.blocks.append((ring_source(s), self.down, self.up.reshape(self.shapes[1])))

    def empty(self, after):
        n = lax.axis_size("fs")
        (rows, inner), (outer, cols) = self.shapes
        index, value, output = self.blocks[0]
        value, output, _ = lax.optimization_barrier((value, output, after))
        return (
            put(jnp.zeros((rows * n, inner), f16), value, index * rows, 0),
            put(jnp.zeros((outer, cols * n), f16), output, index * cols, 1),
        )

    def whole(self, value, output):
        rows, cols = self.shapes[0][0], self.shapes[1][1]
        for index, v, o in self.blocks[1:-1]:
            value = put(value, v, index * rows, 0)
            output = put(output, o, index * cols, 1)
        return value, output


def moments(projected, clip_factor, first_old, second_old):
    scaled = clip_factor * projected
    first_new = first_decay * first_old + (1.0 - first_decay) * scaled
    second_new = second_decay * second_old + (1.0 - second_decay) * scaled * scaled
    return first_new, second_new, first_new * lax.rsqrt(second_new)


def update(
    first_map,
    second_map,
    lambda_head,
    head_gain,
    cot_output,
    layer_input,
    cot_values,
    factor_value,
    factor_output,
    weight_value,
    weight_output,
    first_value,
    second_value,
    first_output,
    second_output,
):
    n, t = lax.axis_size("fs"), lax.axis_size("tp")
    column = lax.axis_index("tp")
    rank = factor_value.shape[1]
    part = 2 * rank // t
    half = t // 2

    first = column % half * part
    own = jnp.where(
        column < half,
        lax.dynamic_slice_in_dim(factor_value, first, part, 1),
        lax.dynamic_slice_in_dim(factor_output, first, part, 1),
    )
    blocks, places = blocks_fs(own)
    ring = Ring((weight_value * weight_scale).astype(f16), (weight_output * weight_scale).astype(f16))
    while ring.step < ring.steps:
        ring.start()
    lines, first_map, second_map = lax.optimization_barrier((blocks[: n // 2], first_map, second_map))
    blocks = lines + blocks[n // 2 :]
    heads_out = head_output(first_map, second_map, lambda_head, head_gain)
    mapped, piece = map_tokens(blocks, places, column // half, (layer_input, cot_output))
    mapped = blocks_tp(mapped)
    keep, send, peak = low_rank(mapped, (cot_values, heads_out))
    packed = pack(send, scale_of(peak))
    packed = swap(packed, "fs", 1)
    wides = ring.empty(peak)
    came, power = unpack(packed, send.shape)
    power = scale_of(peak + jnp.exp2(15.0 - power))
    pieces = blocks_tp(piece)
    sums = add_blocks(keep, came)
    packed = [pack(sums[k], power) for k in range(1, n // 2)]
    packed = [shift(p, "fs", 2 * (k + 1)) for k, p in enumerate(packed)]
    low = sums[0]
    for p in packed:
        low = low + unpack(p, low.shape)[0]
    square = jnp.sum(low * low)
    squares = lax.all_to_all(
        jnp.broadcast_to(square, (n * t, 1, 128)), ("fs", "tp"), 0, 0, tiled=False
    )
    pieces = jnp.stack(pieces)
    pieces = jnp.stack([pieces[column ^ c] for c in range(t)])
    pieces, squares = lax.optimization_barrier((pieces, squares))
    total = jnp.sum(squares[:, 0, 0])
    clip_factor = jnp.minimum(1.0, math.sqrt(rank * cot_values.shape[1] * t) * lax.rsqrt(total + norm_epsilon))
    first_v, second_v, ratio_value = moments(low[0], clip_factor, first_value, second_value)
    first_o, second_o, ratio_output = moments(low[1], clip_factor, first_output, second_output)

    ratio = jnp.stack([ratio_value, ratio_output]) * ratio_scale
    ratios = gather_fs(ratio.astype(f16)).reshape(n, 2, rank // n, -1).astype(f32)
    ratios = ratios * (-learn_rate / ratio_scale)

    def step(which):
        high, low = split(ratios[:, which].reshape(rank, -1))
        return jnp.concatenate([high, low], axis=0)

    step_value, step_output = step(0), step(1)

    def twice(x):
        return jnp.concatenate([x, x], axis=1)

    wide_value, wide_output = ring.whole(*wides)
    new_value = weight_value + dot(twice(factor_value), step_value, ((1,), (0,)))
    new_output = weight_output + dot(step_output, twice(factor_output), ((0,), (1,)))
    whole_value = jnp.concatenate([pieces[c] for c in range(half)] * 2, axis=1)
    whole_output = jnp.concatenate([pieces[c] for c in range(half, t)] * 2, axis=1)

    def value_rows(held, factor):
        return (held.astype(f32) * (1.0 / weight_scale) + dot(factor, step_value, ((1,), (0,)))).astype(bf16)

    def output_cols(held, factor):
        return (held.astype(f32) * (1.0 / weight_scale) + dot(step_output, factor, ((0,), (1,)))).astype(bf16)

    def rows_of(factor, count):
        return lax.dynamic_slice_in_dim(factor, index * count, count, 0)

    index, far_value, far_output = ring.blocks[-1]
    rows, cols = far_value.shape[0], far_output.shape[1]
    copy_output = output_cols(wide_output, whole_output)
    far_output, copy_output = lax.optimization_barrier((far_output, copy_output))
    far_output = output_cols(far_output, rows_of(whole_output, cols))
    copy_output = put(copy_output, far_output, index * cols, 1)
    copy_value = value_rows(wide_value, whole_value)
    far_value, copy_value = lax.optimization_barrier((far_value, copy_value))
    far_value = value_rows(far_value, rows_of(whole_value, rows))
    copy_value = put(copy_value, far_value, index * rows, 0)
    return (
        new_value,
        first_v,
        second_v,
        copy_value,
        new_output,
        first_o,
        second_o,
        copy_output,
    )


def solution(mesh):
    placed = (
        P("fs", "tp"),
        P("fs", "tp"),
        P("tp"),
        P("tp"),
        P("fs", None),
        P("fs", None),
        P("fs", "tp"),
        P("fs", None),
        P("fs", None),
        P("fs", "tp"),
        P("tp", "fs"),
        P("fs", "tp"),
        P("fs", "tp"),
        P("fs", "tp"),
        P("fs", "tp"),
    )
    return jax.shard_map(
        update,
        mesh=mesh,
        in_specs=placed,
        out_specs=(
            P("fs", "tp"),
            P("fs", "tp"),
            P("fs", "tp"),
            P(None, "tp"),
            P("tp", "fs"),
            P("fs", "tp"),
            P("fs", "tp"),
            P("tp", None),
        ),
        check_vma=False,
    )
```

```python
import math

import jax
import jax.numpy as jnp
from jax import lax
from jax.experimental import pallas as pl
from jax.experimental.pallas import tpu as pltpu
from jax.sharding import PartitionSpec as P


norm_epsilon = 1e-06
first_decay = 0.9
second_decay = 0.95
learn_rate = 0.1
weight_scale = 2.0**13
ratio_scale = 2.0**10


f32, bf16, f16 = jnp.float32, jnp.bfloat16, jnp.float16


SMEM = pl.BlockSpec(memory_space=pltpu.SMEM)
VMEM = pl.BlockSpec(memory_space=pltpu.VMEM)
ANY = pl.BlockSpec(memory_space=pl.ANY)


def head_output(first_map, second_map, lambda_head, head_gain):
    heads_here = lambda_head.shape[0]
    count, cols = first_map.shape
    head_width = cols // heads_here
    parts = 8
    rows = count // parts

    def kernel(spread, first, second, gain, out):
        @pl.loop(0, parts)
        def _(p):
            span = pl.ds(pl.multiple_of(p * rows, rows), rows)
            for h in range(heads_here):
                lanes = slice(h * head_width, (h + 1) * head_width)
                differ = first[span, lanes].astype(f32) - spread[h] * second[span, lanes].astype(f32)
                mean = jnp.mean(differ * differ, -1, keepdims=True)
                scaled = differ * lax.rsqrt(mean + norm_epsilon) * gain[:, lanes]
                out[span, lanes] = scaled.astype(bf16)

    return pl.pallas_call(
        kernel,
        out_shape=jax.ShapeDtypeStruct((count, cols), bf16),
        in_specs=[SMEM, VMEM, VMEM, VMEM],
        out_specs=VMEM,
        cost_estimate=pl.CostEstimate(flops=2000 * count * cols, bytes_accessed=6 * count * cols, transcendentals=0),
        compiler_params=pltpu.CompilerParams(vmem_limit_bytes=8 * 2**20),
        name="head_output",
    )(lambda_head, first_map, second_map, head_gain[None])


def split(x):
    high = lax.reduce_precision(x, 8, 7)
    return high.astype(bf16), (x - high).astype(bf16)


def dot(a, b, dims):
    return lax.dot_general(a, b, (dims, ((), ())), preferred_element_type=f32)


def swap(x, axis, bit):
    n = lax.axis_size(axis)
    return lax.ppermute(x, axis, [(i, i ^ bit) for i in range(n)])


def put(whole, block, index, dim=0):
    return lax.dynamic_update_slice_in_dim(whole, block, index, dim)


def blocks_fs(x):
    n = lax.axis_size("fs")
    half = n // 2
    me = lax.axis_index("fs")
    outer, inner = me // 2, me % 2
    line = [x] + [swap(x, "fs", 2 * k) for k in range(1, half)]
    across = [swap(block, "fs", 1) for block in line]
    places = [(outer ^ k) * 2 for k in range(half)]
    return line + across, [p + inner for p in places] + [p + 1 - inner for p in places]


def blocks_tp(x):
    t = lax.axis_size("tp")
    bit = t // 2
    found = {0: x}
    while bit:
        for r in sorted(found):
            found[r | bit] = swap(found[r], "tp", bit)
        bit //= 2
    return [found[r] for r in range(t)]


def gather_fs(x):
    n = lax.axis_size("fs")
    half = n // 2
    me = lax.axis_index("fs")
    outer, inner = me // 2, me % 2
    arrived = [x] + [swap(x, "fs", 2 * k) for k in range(1, half)]
    mine = jnp.stack(arrived)
    bit = half // 2
    while bit:
        pairs = mine.reshape((half // (2 * bit), 2, bit) + x.shape)
        mine = jnp.where((outer // bit) % 2 == 0, pairs, pairs[:, ::-1]).reshape(mine.shape)
        bit //= 2
    other = swap(mine, "fs", 1)
    lower = jnp.where(inner == 0, mine, other)
    upper = jnp.where(inner == 0, other, mine)
    return jnp.stack([lower, upper], axis=1)


def map_tokens(blocks, places, which, tokens):
    n = len(blocks)
    count, width = tokens[0].shape
    deep, part = blocks[0].shape

    parts = 4
    rows = count // parts

    def kernel(at, *refs):
        block_refs, token_refs = refs[:n], refs[n : n + 2]
        product, whole, held, sems = refs[n + 2 :]
        spans = [pl.ds(pl.multiple_of(at[b] * deep, deep), deep) for b in range(n)]

        def fetch(source, p):
            here = pl.ds(p * rows, rows)
            return pltpu.make_async_copy(source.at[here], held.at[here], sems.at[p])

        for w in range(2):

            @pl.when(at[n] == w)
            def _():
                for p in range(parts):
                    fetch(token_refs[w], p).start()

        for b in range(n):
            whole[spans[b], :] = block_refs[b][...]
        for p in range(parts):
            fetch(token_refs[0], p).wait()
            here = slice(p * rows, (p + 1) * rows)
            total = jnp.dot(held[here], whole[...], preferred_element_type=f32)
            product[here, :] = total

    at = jnp.stack([p.astype(jnp.int32) for p in places + [which]])
    return pl.pallas_call(
        kernel,
        out_shape=(
            jax.ShapeDtypeStruct((count, part), f32),
            jax.ShapeDtypeStruct((width, part), bf16),
        ),
        in_specs=[SMEM] + [VMEM] * n + [ANY] * 2,
        out_specs=(VMEM, VMEM),
        scratch_shapes=[pltpu.VMEM((count, width), bf16), pltpu.SemaphoreType.DMA((parts,))],
        cost_estimate=pl.CostEstimate(flops=2 * count * width * 256, bytes_accessed=2 * count * width, transcendentals=0),
        compiler_params=pltpu.CompilerParams(vmem_limit_bytes=56 * 2**20),
        name="map_tokens",
    )(at, *blocks, *tokens)


def low_rank(mapped, rights):
    t, n = lax.axis_size("tp"), lax.axis_size("fs")
    count, part = mapped[0].shape
    cols = rights[0].shape[1]
    rank = part * t // 2
    rows = rank // n

    def kernel(at, *refs):
        mapped_refs, right_refs = refs[:t], refs[t : t + 2]
        keep, send, peak, both, total = refs[t + 2 :]
        for m in range(2):
            both[m] = right_refs[m][...]
        for r in range(t):
            m, h = at[r] // (t // 2), at[r] % (t // 2)
            x = mapped_refs[r][...].T
            high = x.astype(bf16)
            low = (x - high.astype(f32)).astype(bf16)
            right = both[m]
            total[m, pl.ds(pl.multiple_of(h * part, part), part), :] = jnp.dot(
                high, right, preferred_element_type=f32
            ) + jnp.dot(low, right, preferred_element_type=f32)
        top = jnp.zeros((8, cols), f32)
        for m in range(2):
            tall = jnp.abs(total[m])
            top = jnp.maximum(top, jnp.max(tall.reshape(rank // 8, 8, cols), axis=0))
        peak[...] = jnp.max(top, axis=(0, 1), keepdims=True) + jnp.zeros((8, cols), f32)
        for k in range(n // 2):
            o = at[t + 1] ^ k
            for m in range(2):
                first = pl.multiple_of((2 * o + at[t]) * rows, rows)
                keep[k, m] = total[m, pl.ds(first, rows), :]
                other = pl.multiple_of((2 * o + 1 - at[t]) * rows, rows)
                send[k, m] = total[m, pl.ds(other, rows), :]

    me = lax.axis_index("tp")
    here = lax.axis_index("fs")
    at = jnp.stack([me ^ r for r in range(t)] + [here % 2, here // 2]).astype(jnp.int32)
    shape = jax.ShapeDtypeStruct((n // 2, 2, rows, cols), f32)
    return pl.pallas_call(
        kernel,
        out_shape=(shape, shape, jax.ShapeDtypeStruct((8, cols), f32)),
        in_specs=[SMEM] + [VMEM] * (t + 2),
        out_specs=(VMEM, VMEM, VMEM),
        scratch_shapes=[pltpu.VMEM((2, count, cols), bf16), pltpu.VMEM((2, rank, cols), f32)],
        cost_estimate=pl.CostEstimate(flops=8 * count * rank * cols, bytes_accessed=4 * rank * cols, transcendentals=0),
        compiler_params=pltpu.CompilerParams(vmem_limit_bytes=14 * 2**20),
        name="low_rank",
    )(at, *mapped, *rights)


def scale_of(peak):
    return jnp.clip(jnp.floor(14.0 - jnp.log2(jnp.maximum(peak, 1e-30))), -100.0, 100.0)


def pack(x, power):
    body = (x.reshape(-1, x.shape[-1]) * jnp.exp2(power[:1])).astype(f16)
    return jnp.concatenate([body, power.astype(f16)], axis=0)


def unpack(packed, shape):
    power = packed[-8:].astype(f32)
    return (packed[:-8].astype(f32) * jnp.exp2(-power[:1])).reshape(shape), power


def ring_tables():
    n = lax.axis_size("fs")
    order = list(range(0, n, 2)) + list(range(n - 1, 0, -2))
    ahead = [(order[k], order[(k + 1) % n]) for k in range(n)]
    back = [(b, a) for a, b in ahead]
    return ahead, back


def ring_source(steps):
    n = lax.axis_size("fs")
    me = lax.axis_index("fs")
    place = jnp.where(me % 2 == 0, me // 2, n - 1 - me // 2)
    place = (place - steps) % n
    return jnp.where(place < n // 2, 2 * place, 2 * (n - 1 - place) + 1)


class Ring:
    def __init__(self, value, output):
        n = lax.axis_size("fs")
        self.shapes = (value.shape, output.shape)
        self.ahead, self.back = ring_tables()
        self.down = self.up = jnp.stack([value, output.reshape(value.shape)])
        self.steps = n // 2
        self.step = 0
        self.blocks = [(lax.axis_index("fs"), value, output)]

    def start(self):
        self.step += 1
        self.send()
        self.keep()

    def send(self):
        if self.step < self.steps:
            self.down = lax.ppermute(self.down, "fs", self.ahead)
            self.up = lax.ppermute(self.up, "fs", self.back)
        else:
            self.down = lax.ppermute(self.down[0], "fs", self.ahead)
            self.up = lax.ppermute(self.up[1], "fs", self.back)

    def keep(self):
        s = self.step
        if s < self.steps:
            for k, block in ((s, self.down), (-s, self.up)):
                self.blocks.append((ring_source(k), block[0], block[1].reshape(self.shapes[1])))
        else:
            self.blocks.append((ring_source(s), self.down, self.up.reshape(self.shapes[1])))

    def empty(self, after):
        n = lax.axis_size("fs")
        (rows, inner), (outer, cols) = self.shapes
        index, value, output = self.blocks[0]
        value, output, _ = lax.optimization_barrier((value, output, after))
        return (
            put(jnp.zeros((rows * n, inner), f16), value, index * rows, 0),
            put(jnp.zeros((outer, cols * n), f16), output, index * cols, 1),
        )

    def whole(self, value, output):
        rows, cols = self.shapes[0][0], self.shapes[1][1]
        steps = list(range(1, self.steps))
        for s in steps[1:2] + steps[:1] + steps[2:]:
            for index, v, o in self.blocks[2 * s - 1 : 2 * s + 1]:
                value = put(value, v, index * rows, 0)
                output = put(output, o, index * cols, 1)
        return value, output


def moments(projected, clip_factor, first_old, second_old):
    scaled = clip_factor * projected
    first_new = first_decay * first_old + (1.0 - first_decay) * scaled
    second_new = second_decay * second_old + (1.0 - second_decay) * scaled * scaled
    return first_new, second_new, first_new * lax.rsqrt(second_new)


def update(
    first_map,
    second_map,
    lambda_head,
    head_gain,
    cot_output,
    layer_input,
    cot_values,
    factor_value,
    factor_output,
    weight_value,
    weight_output,
    first_value,
    second_value,
    first_output,
    second_output,
):
    n, t = lax.axis_size("fs"), lax.axis_size("tp")
    column = lax.axis_index("tp")
    rank = factor_value.shape[1]
    part = 2 * rank // t
    half = t // 2

    first = column % half * part
    own = jnp.where(
        column < half,
        lax.dynamic_slice_in_dim(factor_value, first, part, 1),
        lax.dynamic_slice_in_dim(factor_output, first, part, 1),
    )
    blocks, places = blocks_fs(own)
    ring = Ring((weight_value * weight_scale).astype(f16), (weight_output * weight_scale).astype(f16))
    while ring.step < ring.steps:
        ring.start()
    lines, first_map, second_map = lax.optimization_barrier((blocks[: n // 2], first_map, second_map))
    blocks = lines + blocks[n // 2 :]
    heads_out = head_output(first_map, second_map, lambda_head, head_gain)
    mapped, piece = map_tokens(blocks, places, column // half, (layer_input, cot_output))
    mapped = blocks_tp(mapped)
    keep, send, peak = low_rank(mapped, (cot_values, heads_out))
    packed = pack(send, scale_of(peak))
    packed = swap(packed, "fs", 1)
    wides = ring.empty(peak)
    came, power = unpack(packed, send.shape)
    power = scale_of(peak + jnp.exp2(15.0 - power))
    pieces = blocks_tp(piece)
    sums = keep + came
    packed = [pack(sums[k], power) for k in range(1, n // 2)]
    packed = [swap(p, "fs", 2 * (k + 1)) for k, p in enumerate(packed)]
    low = sums[0]
    for p in packed:
        low = low + unpack(p, low.shape)[0]
    square = jnp.sum(low * low)
    squares = lax.all_to_all(
        jnp.broadcast_to(square, (n * t, 1, 128)), ("fs", "tp"), 0, 0, tiled=False
    )
    pieces = jnp.stack(pieces)
    pieces = jnp.stack([pieces[column ^ c] for c in range(t)])
    pieces, squares = lax.optimization_barrier((pieces, squares))
    total = jnp.sum(squares[:, 0, 0])
    clip_factor = jnp.minimum(1.0, math.sqrt(rank * cot_values.shape[1] * t) * lax.rsqrt(total + norm_epsilon))
    first_v, second_v, ratio_value = moments(low[0], clip_factor, first_value, second_value)
    first_o, second_o, ratio_output = moments(low[1], clip_factor, first_output, second_output)

    ratio = jnp.stack([ratio_value, ratio_output]) * ratio_scale
    ratios = gather_fs(ratio.astype(f16)).reshape(n, 2, rank // n, -1).astype(f32)
    ratios = ratios * (-learn_rate / ratio_scale)

    def step(which):
        high, low = split(ratios[:, which].reshape(rank, -1))
        return jnp.concatenate([high, low], axis=0)

    step_value, step_output = step(0), step(1)

    def twice(x):
        return jnp.concatenate([x, x], axis=1)

    wide_value, wide_output = ring.whole(*wides)
    new_value = weight_value + dot(twice(factor_value), step_value, ((1,), (0,)))
    new_output = weight_output + dot(step_output, twice(factor_output), ((0,), (1,)))
    whole_value = jnp.concatenate([pieces[c] for c in range(half)] * 2, axis=1)
    whole_output = jnp.concatenate([pieces[c] for c in range(half, t)] * 2, axis=1)

    def value_rows(held, factor):
        return (held.astype(f32) * (1.0 / weight_scale) + dot(factor, step_value, ((1,), (0,)))).astype(bf16)

    def output_cols(held, factor):
        return (held.astype(f32) * (1.0 / weight_scale) + dot(step_output, factor, ((0,), (1,)))).astype(bf16)

    def rows_of(factor, count):
        return lax.dynamic_slice_in_dim(factor, index * count, count, 0)

    index, far_value, far_output = ring.blocks[-1]
    rows, cols = far_value.shape[0], far_output.shape[1]
    copy_output = output_cols(wide_output, whole_output)
    far_output, copy_output = lax.optimization_barrier((far_output, copy_output))
    far_output = output_cols(far_output, rows_of(whole_output, cols))
    copy_output = put(copy_output, far_output, index * cols, 1)
    copy_value = value_rows(wide_value, whole_value)
    far_value, copy_value = lax.optimization_barrier((far_value, copy_value))
    far_value = value_rows(far_value, rows_of(whole_value, rows))
    copy_value = put(copy_value, far_value, index * rows, 0)
    return (
        new_value,
        first_v,
        second_v,
        copy_value,
        new_output,
        first_o,
        second_o,
        copy_output,
    )


def solution(mesh):
    placed = (
        P("fs", "tp"),
        P("fs", "tp"),
        P("tp"),
        P("tp"),
        P("fs", None),
        P("fs", None),
        P("fs", "tp"),
        P("fs", None),
        P("fs", None),
        P("fs", "tp"),
        P("tp", "fs"),
        P("fs", "tp"),
        P("fs", "tp"),
        P("fs", "tp"),
        P("fs", "tp"),
    )
    return jax.shard_map(
        update,
        mesh=mesh,
        in_specs=placed,
        out_specs=(
            P("fs", "tp"),
            P("fs", "tp"),
            P("fs", "tp"),
            P(None, "tp"),
            P("tp", "fs"),
            P("fs", "tp"),
            P("fs", "tp"),
            P("tp", None),
        ),
        check_vma=False,
    )
```
